32 devices in a mesh: ep: 8 (over z, core), tp: 4 (over y, x).
Axes of the slice: x: 2, y: 2, z: 4, core: 2. Of those that a mesh axis runs over, the one named last changes fastest.
Arguments:
- recurrence_queries: bfloat16 [4096, 2048], P('ep', 'tp'), may hold values from -6 to 6
- forget_preact: bfloat16 [4096, 2048], P('ep', 'tp')
- recurrence_values: bfloat16 [4096, 2048], P('ep', 'tp'), may hold values from -6 to 6
- output_gate_preact: bfloat16 [4096, 2048], P('ep', 'tp'), may hold values from -6 to 6
- forget_floor_logits: float32 [2048], P('tp')
- surge_log_decay: float32 [4096, 16], P('ep', 'tp'), may hold values from -0.7 to 0
- head_norm_gain: float32 [128], replicated, may hold values from 0.1 to 1.9
- recurrence_out_weight: bfloat16 [2048, 2048], P(None, 'tp'), may hold values from -0.125 to 0.125
- second_micro_rows: bfloat16 [1024, 2048], P('ep'), may hold values from -6 to 6
- expert_norm_gain: float32 [2048], replicated, may hold values from 0.1 to 1.9
- row_group_index: int32 [1024], P('ep'), may hold values from 0 to 3, as said below
- group_expert_index: int32 [1024, 2], P('ep'), may hold values from 0 to 7, as said below
- chosen_expert_weight: float32 [1024, 2], P('ep'), may hold values from 0.2 to 1
- expert_gate_weight: bfloat16 [32, 2048, 4096], P('ep', None, 'tp'), may hold values from -0.125 to 0.125
- expert_up_weight: bfloat16 [32, 2048, 4096], P('ep', None, 'tp'), may hold values from -0.125 to 0.125
- expert_down_weight: bfloat16 [32, 4096, 2048], P('ep', None, 'tp'), may hold values from -0.09375 to 0.09375
Outputs:
- mixed: bfloat16 [4096, 2048], P('ep', 'tp')
- expert_out: bfloat16 [1024, 2048], P('ep', 'tp')
The draws below stay inside these ranges and needn't reach their ends.
Inputs may be any that keep to these rules, and one draw needn't show every extreme that they name: group_expert_index names two different experts of the row's group; the expert's number is row_group_index * 8 + group_expert_index. Among the rows of one index of ep no expert is named more than 12 times, and some expert exactly 12 times. `group_expert_index`: the two entries of a row differ.
All inputs are finite; a program needn't handle non-finite values.
Results may differ from the reference program's by a relative error of at most 0.009.
Values may be sent and summed in bfloat16 or wider, within the bound.
A program may use at most 128 MiB of HBM per device.

```python
import math
import jax
import jax.numpy as jnp
from jax import lax

D = 2048
HEADS = 16
KEY_DIM = 128
VAL_DIM = 128
BLOCK = 64
EXPERTS = 32
GROUPS = 4
FF = 4096
TOK_M = 512
LENGTH = 4096
EXP_ROWS = 128
ALL_ROWS = 1024
CAP = 12
N_EP = 8


def draw_forget_preact(key, part):
    array_shape = (LENGTH, HEADS * KEY_DIM)
    base = jax.random.normal(jax.random.fold_in(key, 1), array_shape, jnp.float32)
    shift = jax.random.uniform(jax.random.fold_in(key, 2), (LENGTH // TOK_M, 1), jnp.float32, -1.5, 1.5)
    return (base + jnp.repeat(shift, TOK_M, axis=0)).astype(jnp.bfloat16)


def draw_forget_floor_logits(key, part):
    share = 0.5
    slow = jax.random.uniform(jax.random.fold_in(key, 21), (HEADS, 1), jnp.float32) < share
    spread = jax.random.uniform(jax.random.fold_in(key, 22), (HEADS, KEY_DIM), jnp.float32, 0.5, 2.0) / LENGTH
    quick = jnp.exp(jax.random.uniform(jax.random.fold_in(key, 23), (HEADS, KEY_DIM), jnp.float32, math.log(0.02), math.log(0.066)))
    rate = jnp.where(slow, spread, quick)
    return jnp.log((1.0 - rate) / rate).reshape(-1).astype(jnp.float32)


def draw_surge_log_decay(key, part):
    hit = jax.random.uniform(jax.random.fold_in(key, 31), (LENGTH, HEADS), jnp.float32) < 6.0 / LENGTH
    depth = jnp.log(jax.random.uniform(jax.random.fold_in(key, 32), (LENGTH, HEADS), jnp.float32, 0.5, 0.8))
    return jnp.where(hit, depth, 0.0).astype(jnp.float32)


def route_parts(key):
    block_total = ALL_ROWS // EXP_ROWS
    unit_rows = EXP_ROWS // 32
    patterns = jnp.array([[12, 8, 6, 6], [12, 10, 6, 4]], jnp.int32) * unit_rows
    chosen = jax.random.randint(jax.random.fold_in(key, 11), (block_total,), 0, 2)

    def one_block(index):
        sub_key = jax.random.fold_in(key, 100 + index)
        counts = patterns[chosen[index]]
        counts = counts[jax.random.permutation(jax.random.fold_in(sub_key, 1), 4)]
        bounds = jnp.cumsum(counts)
        position = jnp.arange(EXP_ROWS, dtype=jnp.int32)
        group = jnp.sum((position[:, None] >= bounds[None, :]).astype(jnp.int32), axis=1)
        begins = bounds - counts
        within = position - begins[group]
        orders = jnp.stack([jax.random.permutation(jax.random.fold_in(sub_key, 2 + g), 8) for g in range(4)])
        first = orders[group, within % 8]
        second = orders[group, (within + 4) % 8]
        row_perm = jax.random.permutation(jax.random.fold_in(sub_key, 9), EXP_ROWS)
        inverse = jnp.argsort(row_perm)
        return (group[inverse], jnp.stack([first, second], axis=1)[inverse])
    groups, local_sets = jax.vmap(one_block)(jnp.arange(block_total))
    return (groups.reshape(-1).astype(jnp.int32), local_sets.reshape(-1, 2).astype(jnp.int32))


def draw_row_group_index(key, part):
    return route_parts(jax.random.fold_in(key, 7))[0]


def draw_group_expert_index(key, part):
    return route_parts(jax.random.fold_in(key, 7))[1]


def block_scale(own_key, dims, split, low, largest):
    factor_of, own = 1.0, jax.random.fold_in(own_key, 6)
    for axis_at, shards_of in split:
        draws = jnp.exp(jax.random.uniform(jax.random.fold_in(own, axis_at), (shards_of,), jnp.float32, low / len(split), largest / len(split)))
        factor_of = factor_of * jnp.repeat(draws, dims[axis_at] // shards_of).reshape([-1 if axis == axis_at else 1 for axis in range(len(dims))])
    return factor_of


def bell_draw(key, dims, scale, reach, shards=(), kind=jnp.bfloat16):
    result = scale * jax.random.normal(key, dims, jnp.float32)
    if shards:
        result = result * block_scale(key, dims, shards, -0.22, 0.18)
    return jnp.clip(result, -reach, reach).astype(kind)


def setup_inputs(seed: int = 0) -> dict:
    splits = jax.random.split(jax.random.key(seed), 17)
    return {
        "recurrence_queries": bell_draw(splits[0], (LENGTH, HEADS * KEY_DIM), 1.0, 6.0, ((0, 8), (1, 4))),
        "forget_preact": draw_forget_preact(jax.random.fold_in(splits[16], 71), 0),
        "recurrence_values": bell_draw(splits[2], (LENGTH, HEADS * VAL_DIM), 1.0, 6.0, ((0, 8), (1, 4))),
        "output_gate_preact": bell_draw(splits[3], (LENGTH, HEADS * VAL_DIM), 1.0, 6.0, ((0, 8), (1, 4))),
        "forget_floor_logits": draw_forget_floor_logits(jax.random.fold_in(splits[16], 71), 0),
        "surge_log_decay": draw_surge_log_decay(jax.random.fold_in(splits[16], 71), 0),
        "head_norm_gain": jnp.clip(1.0 + 0.18 * jax.random.normal(splits[6], (VAL_DIM,), jnp.float32), 0.1, 1.9),
        "recurrence_out_weight": bell_draw(splits[7], (HEADS * VAL_DIM, D), (HEADS * VAL_DIM) ** -0.5, 0.125, ((1, 4),)),
        "second_micro_rows": bell_draw(splits[8], (ALL_ROWS, D), 1.0, 6.0, ((0, 8),)),
        "expert_norm_gain": jnp.clip(1.0 + 0.18 * jax.random.normal(splits[9], (D,), jnp.float32), 0.1, 1.9),
        "row_group_index": draw_row_group_index(jax.random.fold_in(splits[16], 71), 0),
        "group_expert_index": draw_group_expert_index(jax.random.fold_in(splits[16], 71), 0),
        "chosen_expert_weight": jnp.clip(0.2 + 0.8 * jax.random.uniform(splits[12], (ALL_ROWS, 2), jnp.float32) ** block_scale(splits[12], (ALL_ROWS, 2), ((0, 8),), -0.2, 0.2), 0.2, 1.0),
        "expert_gate_weight": bell_draw(splits[13], (EXPERTS, D, FF), D ** -0.5, 0.125, ((0, 8), (2, 4))),
        "expert_up_weight": bell_draw(splits[14], (EXPERTS, D, FF), D ** -0.5, 0.125, ((0, 8), (2, 4))),
        "expert_down_weight": bell_draw(splits[15], (EXPERTS, FF, D), FF ** -0.5, 0.09375, ((0, 8), (2, 4))),
    }


NORM_EPS = 1e-06
EXACT_PRECISION = lax.Precision.HIGHEST

def block_recurrence(query_activated, key_in, value_act, forget_log_value, state_init):
    block_len = query_activated.shape[1]
    causal = (jnp.arange(block_len)[:, None] >= jnp.arange(block_len)[None, :])[:, :, None, None]

    def block_step(current_state, block_inputs):
        query_tile, key_tile, value_tile, g_block = block_inputs
        running_total_sum = jnp.cumsum(g_block, axis=0)
        state_carried_out = jnp.einsum('cra,ran->crn', query_tile * jnp.exp(running_total_sum), current_state, precision=EXACT_PRECISION)
        relative = jnp.where(causal, running_total_sum[:, None] - running_total_sum[None, :], 0.0)
        decays = jnp.where(causal, jnp.exp(relative), 0.0)
        scores = jnp.einsum('thk,tshk,shk->hts', query_tile, decays, key_tile, precision=EXACT_PRECISION)
        output = state_carried_out + jnp.einsum('hts,shv->thv', scores, value_tile, precision=EXACT_PRECISION)
        final_log_value = running_total_sum[-1]
        current_state = jnp.exp(final_log_value)[:, :, None] * current_state + jnp.einsum('ceu,cex->eux', key_tile * jnp.exp(final_log_value[None] - running_total_sum), value_tile, precision=EXACT_PRECISION)
        return (current_state, output)
    return lax.scan(block_step, state_init, (query_activated, key_in, value_act, forget_log_value))

def token_mixing_layer(recurrence_queries, forget_preact, recurrence_values, output_gate_preact, forget_floor_logits, surge_log_decay, head_norm_gain, recurrence_out_weight):
    sequence_length = recurrence_queries.shape[0]
    number_of_heads = surge_log_decay.shape[1]
    key_feature_width = recurrence_queries.shape[1] // number_of_heads
    val_dim = recurrence_values.shape[1] // number_of_heads
    rate = jax.nn.sigmoid(-forget_floor_logits)
    input_gate_value = rate * jax.nn.sigmoid(-forget_preact.astype(jnp.float32))
    forget_log_value = jnp.log1p(-input_gate_value).reshape(sequence_length, number_of_heads, key_feature_width) + surge_log_decay[:, :, None]
    query_activated = jax.nn.silu(recurrence_queries.astype(jnp.float32)).reshape(sequence_length, number_of_heads, key_feature_width)
    key_in = input_gate_value.reshape(sequence_length, number_of_heads, key_feature_width)
    value_act = recurrence_values.astype(jnp.float32).reshape(sequence_length, number_of_heads, val_dim)
    block_count = sequence_length // BLOCK

    def to_blocks(array):
        return array.reshape(block_count, BLOCK, number_of_heads, array.shape[-1])
    state_init = jnp.zeros((number_of_heads, key_feature_width, val_dim), jnp.float32)
    _, recur_out = block_recurrence(to_blocks(query_activated), to_blocks(key_in), to_blocks(value_act), to_blocks(forget_log_value), state_init)
    recur_out = recur_out.reshape(sequence_length, number_of_heads, val_dim)
    normed = recur_out * lax.rsqrt(lax.optimization_barrier(jnp.mean(recur_out * recur_out, axis=-1, keepdims=True)) + NORM_EPS) * head_norm_gain
    gate_act = jax.nn.silu(output_gate_preact.astype(jnp.float32)).reshape(sequence_length, number_of_heads, val_dim)
    gated_heads = (normed * gate_act).reshape(sequence_length, number_of_heads * val_dim).astype(jnp.bfloat16)
    return jnp.dot(gated_heads, recurrence_out_weight, preferred_element_type=jnp.float32).astype(jnp.bfloat16)

def routed_experts(second_micro_rows, expert_norm_gain, row_group_index, group_expert_index, chosen_expert_weight, expert_gate_weight, expert_up_weight, expert_down_weight):
    row_count = second_micro_rows.shape[0]
    model_width = second_micro_rows.shape[1]
    expert_count = expert_gate_weight.shape[0]
    per_group = expert_count // GROUPS
    rows_float = second_micro_rows.astype(jnp.float32)
    normed_rows = (rows_float * lax.rsqrt(lax.optimization_barrier(jnp.mean(rows_float * rows_float, axis=-1, keepdims=True)) + NORM_EPS) * expert_norm_gain).astype(jnp.bfloat16)
    expert_choice = (row_group_index[:, None] * per_group + group_expert_index).astype(jnp.int32)
    flat_expert = expert_choice.reshape(-1)
    onehot = (flat_expert[:, None] == jnp.arange(expert_count, dtype=jnp.int32)[None, :]).astype(jnp.int32)
    rank_index = lax.optimization_barrier(jnp.sum((jnp.cumsum(onehot, axis=0) - onehot) * onehot, axis=1)).astype(jnp.int32)
    room_size = N_EP * CAP
    slot_index = (flat_expert * room_size + rank_index).astype(jnp.int32)
    owner_row = jnp.full((expert_count * room_size,), row_count, jnp.int32).at[slot_index].set((jnp.arange(2 * row_count) // 2).astype(jnp.int32))
    padded = jnp.concatenate([normed_rows, jnp.zeros((1, model_width), jnp.bfloat16)], axis=0)

    def expert_block(operands):
        row_index, gate_mat, up_mat, down_mat = operands
        gathered_rows = padded[row_index]
        gate_act = jnp.dot(gathered_rows, gate_mat, preferred_element_type=jnp.float32)
        up_act = jnp.dot(gathered_rows, up_mat, preferred_element_type=jnp.float32)
        expert_hidden = (jax.nn.silu(gate_act) * up_act).astype(jnp.bfloat16)
        return jnp.dot(expert_hidden, down_mat, preferred_element_type=jnp.float32).astype(jnp.bfloat16)
    expert_result = lax.map(expert_block, (owner_row.reshape(expert_count, room_size), expert_gate_weight, expert_up_weight, expert_down_weight))
    picked = expert_result.reshape(expert_count * room_size, model_width)[slot_index]
    picked = picked.reshape(row_count, 2, model_width).astype(jnp.float32)
    return lax.optimization_barrier(jnp.sum(picked * chosen_expert_weight[:, :, None], axis=1)).astype(jnp.bfloat16)

def reference(recurrence_queries, forget_preact, recurrence_values, output_gate_preact, forget_floor_logits, surge_log_decay, head_norm_gain, recurrence_out_weight, second_micro_rows, expert_norm_gain, row_group_index, group_expert_index, chosen_expert_weight, expert_gate_weight, expert_up_weight, expert_down_weight):
    mixed = token_mixing_layer(recurrence_queries, forget_preact, recurrence_values, output_gate_preact, forget_floor_logits, surge_log_decay, head_norm_gain, recurrence_out_weight)
    expert_out = routed_experts(second_micro_rows, expert_norm_gain, row_group_index, group_expert_index, chosen_expert_weight, expert_gate_weight, expert_up_weight, expert_down_weight)
    return (mixed, expert_out)
```

```python
import functools

import jax
import jax.numpy as jnp
import numpy as np
from jax import lax
from jax.experimental import pallas as pl
from jax.experimental.pallas import tpu as pltpu
from jax.sharding import PartitionSpec as P

SPAN = 128
GROUPS = 4
CAP = 12
NORM_EPS = 1e-06
TAIL = 16

NT = (((1,), (1,)), ((), ()))
TN = (((0,), (0,)), ((), ()))


def span_levels(span):
    return span.bit_length() - 1


def log_sum_matrix(span):
    row, col = np.arange(span)[:, None], np.arange(span)[None, :]
    parts = [col <= row, col > row]
    for level in range(span_levels(span)):
        half = 1 << level
        mid = row // (2 * half) * (2 * half) + half - 1
        later = (row & half) != 0
        parts.append(np.where(later, (col > mid) & (col <= row), (col > row) & (col <= mid)))
    stack = np.stack(parts).astype(np.float32)
    return np.concatenate([stack, stack], axis=2)


def high_low(value):
    high = value.astype(jnp.bfloat16)
    return high, (value - high.astype(jnp.float32)).astype(jnp.bfloat16)


def dot(a, b, dims=(((1,), (0,)), ((), ()))):
    return lax.dot_general(a, b, dims, preferred_element_type=jnp.float32)


def recurrence_kernel(heads, q_ref, f_ref, v_ref, floor_ref, surge_ref, sums_ref,
                      out_ref, decayed_ref, ending_ref, state, carry):
    span, width = q_ref.shape
    key, val = width // heads, v_ref.shape[1] // heads

    @pl.when(pl.program_id(0) == 0)
    def _():
        state[...] = jnp.zeros_like(state)
        carry[...] = jnp.zeros_like(carry)

    rate = jax.nn.sigmoid(-floor_ref[...])
    gate = rate * jax.nn.sigmoid(-f_ref[...].astype(jnp.float32))
    surge = surge_ref[...]
    surge = jnp.concatenate(
        [jnp.broadcast_to(surge[:, h:h + 1], (span, key)) for h in range(heads)], axis=1
    )
    forget = jnp.log1p(-gate) + surge
    query = jax.nn.silu(q_ref[...].astype(jnp.float32))
    pieces = jnp.concatenate(high_low(forget), axis=0)

    row = lax.broadcasted_iota(jnp.int32, (span, span), 0)
    col = lax.broadcasted_iota(jnp.int32, (span, span), 1)
    wide_row = lax.broadcasted_iota(jnp.int32, (span, width), 0)

    own = query * gate
    scores = []
    for h in range(heads):
        same = jnp.sum(own[:, h * key:(h + 1) * key], axis=1, keepdims=True)
        scores.append(jnp.where(row == col, same, 0.0))
    for level in range(span_levels(span)):
        half = 1 << level
        decay = jnp.exp(dot(sums_ref[2 + level], pieces))
        side = (jnp.where((wide_row & half) != 0, query, gate) * decay).astype(jnp.bfloat16)
        met = (((row ^ col) >> level) == 1) & ((row & half) != 0)
        for h in range(heads):
            part = side[:, h * key:(h + 1) * key]
            scores[h] = jnp.where(met, dot(part, part, NT), scores[h])

    since = dot(sums_ref[0], pieces)
    until = dot(sums_ref[1], pieces)
    total = since[span - 1:span, :]
    entered = query * jnp.exp(since)
    leaving = (gate * jnp.exp(until)).astype(jnp.bfloat16)
    decayed_ref[...] = (entered * jnp.exp(carry[...])).astype(jnp.bfloat16)
    entered = entered.astype(jnp.bfloat16)
    kept = jnp.exp(total)
    for h in range(heads):
        keys, vals = slice(h * key, (h + 1) * key), slice(h * val, (h + 1) * val)
        values = v_ref[:, vals]
        held = state[h]
        out_ref[:, vals] = dot(scores[h].astype(jnp.bfloat16), values) + dot(
            entered[:, keys], held.astype(jnp.bfloat16), NT
        )
        state[h] = kept[:, keys] * held + dot(values, leaving[:, keys], TN)
    carry[...] = carry[...] + total

    @pl.when(pl.program_id(0) == pl.num_programs(0) - 1)
    def _():
        high, low = high_low(carry[...])
        for h in range(heads):
            keys = slice(h * key, (h + 1) * key)
            ending_ref[h, :val, :] = state[h].astype(jnp.bfloat16)
            ending_ref[h, val:, :] = jnp.concatenate(
                [high[:, keys], low[:, keys], jnp.zeros((TAIL - 2, key), jnp.bfloat16)], axis=0
            )


def finish_kernel(heads, part_ref, decayed_ref, gate_ref, gain_ref, ends_ref, out_ref, state):
    count = ends_ref.shape[0]
    key = decayed_ref.shape[1] // heads
    val = part_ref.shape[1] // heads
    mine = lax.axis_index("ep")

    @pl.when(pl.program_id(0) == 0)
    def _():
        for h in range(heads):
            def hop(place, held, h=h):
                ending = ends_ref[place, h].astype(jnp.float32)
                kept = jnp.exp(ending[val:val + 1] + ending[val + 1:val + 2])
                return jnp.where(place < mine, kept * held + ending[:val], held)

            held = lax.fori_loop(0, count - 1, hop, jnp.zeros((val, key), jnp.float32))
            state[h] = held.astype(jnp.bfloat16)

    gain = gain_ref[...]
    for h in range(heads):
        keys, vals = slice(h * key, (h + 1) * key), slice(h * val, (h + 1) * val)
        out = part_ref[:, vals] + dot(decayed_ref[:, keys], state[h], NT)
        scale = lax.rsqrt(jnp.mean(out * out, axis=-1, keepdims=True) + NORM_EPS)
        gated = out * scale * gain * jax.nn.silu(gate_ref[:, vals].astype(jnp.float32))
        out_ref[:, vals] = gated.astype(jnp.bfloat16)


def mixer_part(queries, forget, values, floor, surge):
    rows, width = queries.shape
    heads = surge.shape[1]
    key, val = width // heads, values.shape[1] // heads
    span = SPAN
    sums = jnp.asarray(log_sum_matrix(span), jnp.bfloat16)
    tile = lambda w: pl.BlockSpec((span, w), lambda i: (i, 0))
    full = lambda *s: pl.BlockSpec(s, lambda i: (0,) * len(s))
    return pl.pallas_call(
        functools.partial(recurrence_kernel, heads),
        grid=(rows // span,),
        in_specs=[tile(width), tile(width), tile(values.shape[1]), full(1, width), tile(heads),
                  full(*sums.shape)],
        out_specs=[tile(values.shape[1]), tile(width), full(heads, val + TAIL, key)],
        out_shape=[
            jax.ShapeDtypeStruct((rows, values.shape[1]), jnp.float32),
            jax.ShapeDtypeStruct((rows, width), jnp.bfloat16),
            jax.ShapeDtypeStruct((heads, val + TAIL, key), jnp.bfloat16),
        ],
        scratch_shapes=[pltpu.VMEM((heads, val, key), jnp.float32), pltpu.VMEM((1, width), jnp.float32)],
        cost_estimate=pl.CostEstimate(flops=12 * 10**9, bytes_accessed=4 * 10**6, transcendentals=0),
        name="recurrence",
    )(queries, forget, values, floor[None, :], surge, sums)


def mixer_finish(part, decayed, gate, gain, ends):
    rows, width = part.shape
    heads = ends.shape[1]
    val, key = ends.shape[2] - TAIL, ends.shape[3]
    span = SPAN
    tile = lambda w: pl.BlockSpec((span, w), lambda i: (i, 0))
    full = lambda *s: pl.BlockSpec(s, lambda i: (0,) * len(s))
    return pl.pallas_call(
        functools.partial(finish_kernel, heads),
        grid=(rows // span,),
        in_specs=[tile(width), tile(decayed.shape[1]), tile(width), full(1, val), full(*ends.shape)],
        out_specs=tile(width),
        out_shape=jax.ShapeDtypeStruct((rows, width), jnp.bfloat16),
        scratch_shapes=[pltpu.VMEM((heads, val, key), jnp.bfloat16)],
        cost_estimate=pl.CostEstimate(flops=4 * 10**9, bytes_accessed=4 * 10**6, transcendentals=0),
        name="finish",
    )(part, decayed, gate, gain[None, :], ends)


def hidden_kernel(x_ref, gate_ref, up_ref, out_ref):
    rows = x_ref[0]
    gate = dot(rows, gate_ref[0])
    up = dot(rows, up_ref[0])
    out_ref[0] = (jax.nn.silu(gate) * up).astype(jnp.bfloat16)


def down_kernel(x_ref, down_ref, out_ref):
    out_ref[0] = dot(x_ref[0], down_ref[0]).astype(jnp.bfloat16)


def expert_call(kernel, rows, weights, tile, name):
    experts, count, depth = rows.shape
    width = weights[0].shape[2]
    tile = min(tile, width)
    size = len(weights) * weights[0].size
    return pl.pallas_call(
        kernel,
        grid=(experts, width // tile),
        in_specs=[pl.BlockSpec((1, count, depth), lambda e, j: (e, 0, 0))]
        + [pl.BlockSpec((1, depth, tile), lambda e, j: (e, 0, j))] * len(weights),
        out_specs=pl.BlockSpec((1, count, tile), lambda e, j: (e, 0, j)),
        out_shape=jax.ShapeDtypeStruct((experts, count, width), jnp.bfloat16),
        cost_estimate=pl.CostEstimate(flops=2 * count * size, bytes_accessed=2 * size, transcendentals=0),
        name=name,
    )(rows, *weights)


def token_mixing_layer(
    recurrence_queries,
    forget_preact,
    recurrence_values,
    output_gate_preact,
    forget_floor_logits,
    surge_log_decay,
    head_norm_gain,
    recurrence_out_weight,
):
    part, decayed, ending = mixer_part(
        recurrence_queries, forget_preact, recurrence_values, forget_floor_logits, surge_log_decay
    )
    ends = lax.all_gather(ending, "ep")
    gated_heads = mixer_finish(part, decayed, output_gate_preact, head_norm_gain, ends)
    return jnp.dot(
        lax.all_gather(gated_heads, "tp", axis=1, tiled=True),
        recurrence_out_weight,
        preferred_element_type=jnp.float32,
    ).astype(jnp.bfloat16)


def routed_experts(
    second_micro_rows,
    expert_norm_gain,
    row_group_index,
    group_expert_index,
    chosen_expert_weight,
    expert_gate_weight,
    expert_up_weight,
    expert_down_weight,
):
    row_count = second_micro_rows.shape[0]
    model_width = second_micro_rows.shape[1]
    columns = model_width // lax.axis_size("tp")
    local_count = expert_gate_weight.shape[0]
    expert_count = local_count * lax.axis_size("ep")
    per_group = expert_count // GROUPS
    rows_float = second_micro_rows.astype(jnp.float32)
    normed_rows = (
        rows_float
        * lax.rsqrt(jnp.mean(rows_float * rows_float, axis=-1, keepdims=True) + NORM_EPS)
        * expert_norm_gain
    ).astype(jnp.bfloat16)
    flat_expert = (row_group_index[:, None] * per_group + group_expert_index).reshape(-1)
    onehot = (flat_expert[:, None] == jnp.arange(expert_count, dtype=jnp.int32)[None, :]).astype(
        jnp.int32
    )
    rank_index = jnp.sum((jnp.cumsum(onehot, axis=0) - onehot) * onehot, axis=1)
    slot_index = flat_expert * CAP + rank_index
    owner_row = (
        jnp.full((expert_count * CAP,), row_count, jnp.int32)
        .at[slot_index]
        .set(jnp.arange(2 * row_count) // 2)
    )
    col_part = lax.dynamic_slice_in_dim(normed_rows, lax.axis_index("tp") * columns, columns, 1)
    padded = jnp.concatenate([col_part, jnp.zeros((1, columns), jnp.bfloat16)], axis=0)
    outgoing = padded[owner_row].reshape(expert_count, CAP, columns)
    arrived = lax.all_to_all(outgoing, "ep", split_axis=0, concat_axis=1, tiled=True)
    arrived = lax.all_gather(arrived, "tp", axis=2, tiled=True)
    hidden = expert_call(
        hidden_kernel, arrived, (expert_gate_weight, expert_up_weight), 256, "hidden"
    )
    hidden = lax.all_gather(hidden, "tp", axis=2, tiled=True)
    result = expert_call(down_kernel, hidden, (expert_down_weight,), 256, "down")
    returned = lax.all_to_all(result, "ep", split_axis=1, concat_axis=0, tiled=True)
    picked = returned.reshape(expert_count * CAP, expert_down_weight.shape[2])[slot_index]
    picked = picked.reshape(row_count, 2, expert_down_weight.shape[2]).astype(jnp.float32)
    return jnp.sum(picked * chosen_expert_weight[:, :, None], axis=1).astype(jnp.bfloat16)


def local(
    recurrence_queries,
    forget_preact,
    recurrence_values,
    output_gate_preact,
    forget_floor_logits,
    surge_log_decay,
    head_norm_gain,
    recurrence_out_weight,
    second_micro_rows,
    expert_norm_gain,
    row_group_index,
    group_expert_index,
    chosen_expert_weight,
    expert_gate_weight,
    expert_up_weight,
    expert_down_weight,
):
    mixed = token_mixing_layer(
        recurrence_queries,
        forget_preact,
        recurrence_values,
        output_gate_preact,
        forget_floor_logits,
        surge_log_decay,
        head_norm_gain,
        recurrence_out_weight,
    )
    expert_out = routed_experts(
        second_micro_rows,
        expert_norm_gain,
        row_group_index,
        group_expert_index,
        chosen_expert_weight,
        expert_gate_weight,
        expert_up_weight,
        expert_down_weight,
    )
    return (mixed, expert_out)


def solution(mesh):
    return jax.shard_map(
        local,
        mesh=mesh,
        in_specs=(
            P("ep", "tp"),
            P("ep", "tp"),
            P("ep", "tp"),
            P("ep", "tp"),
            P("tp"),
            P("ep", "tp"),
            P(),
            P(None, "tp"),
            P("ep", None),
            P(),
            P("ep"),
            P("ep", None),
            P("ep", None),
            P("ep", None, "tp"),
            P("ep", None, "tp"),
            P("ep", None, "tp"),
        ),
        out_specs=(P("ep", "tp"), P("ep", "tp")),
        check_vma=False,
    )
```

```python
import functools

import jax
import jax.numpy as jnp
import numpy as np
from jax import lax
from jax.experimental import pallas as pl
from jax.experimental.pallas import tpu as pltpu
from jax.sharding import PartitionSpec as P

SPAN = 128
GROUPS = 4
CAP = 12
NORM_EPS = 1e-06
TAIL = 16
MESH = pl.DeviceIdType.MESH

NT = (((1,), (1,)), ((), ()))
TN = (((0,), (0,)), ((), ()))


def span_levels(span):
    return span.bit_length() - 1


def log_sum_matrix(span):
    row, col = np.arange(span)[:, None], np.arange(span)[None, :]
    parts = [col <= row, col > row]
    for level in range(span_levels(span)):
        half = 1 << level
        mid = row // (2 * half) * (2 * half) + half - 1
        later = (row & half) != 0
        parts.append(np.where(later, (col > mid) & (col <= row), (col > row) & (col <= mid)))
    stack = np.stack(parts).astype(np.float32)
    return np.concatenate([stack, stack], axis=2)


def high_low(value):
    high = value.astype(jnp.bfloat16)
    return high, (value - high.astype(jnp.float32)).astype(jnp.bfloat16)


def dot(a, b, dims=(((1,), (0,)), ((), ()))):
    return lax.dot_general(a, b, dims, preferred_element_type=jnp.float32)


def recurrence_kernel(heads, q_ref, f_ref, v_ref, floor_ref, surge_ref, sums_ref,
                      out_ref, decayed_ref, ending_ref, state, carry):
    span, width = q_ref.shape
    key, val = width // heads, v_ref.shape[1] // heads

    @pl.when(pl.program_id(0) == 0)
    def _():
        state[...] = jnp.zeros_like(state)
        carry[...] = jnp.zeros_like(carry)

    rate = jax.nn.sigmoid(-floor_ref[...])
    gate = rate * jax.nn.sigmoid(-f_ref[...].astype(jnp.float32))
    surge = surge_ref[...]
    surge = jnp.concatenate(
        [jnp.broadcast_to(surge[:, h:h + 1], (span, key)) for h in range(heads)], axis=1
    )
    forget = jnp.log1p(-gate) + surge
    query = jax.nn.silu(q_ref[...].astype(jnp.float32))
    pieces = jnp.concatenate(high_low(forget), axis=0)

    row = lax.broadcasted_iota(jnp.int32, (span, span), 0)
    col = lax.broadcasted_iota(jnp.int32, (span, span), 1)
    wide_row = lax.broadcasted_iota(jnp.int32, (span, width), 0)

    own = query * gate
    scores = []
    for h in range(heads):
        same = jnp.sum(own[:, h * key:(h + 1) * key], axis=1, keepdims=True)
        scores.append(jnp.where(row == col, same, 0.0))
    for level in range(span_levels(span)):
        half = 1 << level
        decay = jnp.exp(dot(sums_ref[2 + level], pieces))
        side = (jnp.where((wide_row & half) != 0, query, gate) * decay).astype(jnp.bfloat16)
        met = (((row ^ col) >> level) == 1) & ((row & half) != 0)
        for h in range(heads):
            part = side[:, h * key:(h + 1) * key]
            scores[h] = jnp.where(met, dot(part, part, NT), scores[h])

    since = dot(sums_ref[0], pieces)
    until = dot(sums_ref[1], pieces)
    total = since[span - 1:span, :]
    entered = query * jnp.exp(since)
    leaving = (gate * jnp.exp(until)).astype(jnp.bfloat16)
    decayed_ref[...] = (entered * jnp.exp(carry[...])).astype(jnp.bfloat16)
    entered = entered.astype(jnp.bfloat16)
    kept = jnp.exp(total)
    for h in range(heads):
        keys, vals = slice(h * key, (h + 1) * key), slice(h * val, (h + 1) * val)
        values = v_ref[:, vals]
        held = state[h]
        out_ref[:, vals] = dot(scores[h].astype(jnp.bfloat16), values) + dot(
            entered[:, keys], held.astype(jnp.bfloat16), NT
        )
        state[h] = kept[:, keys] * held + dot(values, leaving[:, keys], TN)
    carry[...] = carry[...] + total

    @pl.when(pl.program_id(0) == pl.num_programs(0) - 1)
    def _():
        high, low = high_low(carry[...])
        for h in range(heads):
            keys = slice(h * key, (h + 1) * key)
            ending_ref[h, :val, :] = state[h].astype(jnp.bfloat16)
            ending_ref[h, val:, :] = jnp.concatenate(
                [high[:, keys], low[:, keys], jnp.zeros((TAIL - 2, key), jnp.bfloat16)], axis=0
            )


def finish_kernel(heads, part_ref, decayed_ref, gate_ref, gain_ref, ends_ref, out_ref, state):
    count = ends_ref.shape[0]
    key = decayed_ref.shape[1] // heads
    val = part_ref.shape[1] // heads
    mine = lax.axis_index("ep")

    @pl.when(pl.program_id(0) == 0)
    def _():
        for h in range(heads):
            def hop(place, held, h=h):
                ending = ends_ref[place, h].astype(jnp.float32)
                kept = jnp.exp(ending[val:val + 1] + ending[val + 1:val + 2])
                return jnp.where(place < mine, kept * held + ending[:val], held)

            held = lax.fori_loop(0, count - 1, hop, jnp.zeros((val, key), jnp.float32))
            state[h] = held.astype(jnp.bfloat16)

    gain = gain_ref[...]
    for h in range(heads):
        keys, vals = slice(h * key, (h + 1) * key), slice(h * val, (h + 1) * val)
        out = part_ref[:, vals] + dot(decayed_ref[:, keys], state[h], NT)
        scale = lax.rsqrt(jnp.mean(out * out, axis=-1, keepdims=True) + NORM_EPS)
        gated = out * scale * gain * jax.nn.silu(gate_ref[:, vals].astype(jnp.float32))
        out_ref[:, vals] = gated.astype(jnp.bfloat16)


def mixer_part(queries, forget, values, floor, surge):
    rows, width = queries.shape
    heads = surge.shape[1]
    key, val = width // heads, values.shape[1] // heads
    span = SPAN
    sums = jnp.asarray(log_sum_matrix(span), jnp.bfloat16)
    tile = lambda w: pl.BlockSpec((span, w), lambda i: (i, 0))
    full = lambda *s: pl.BlockSpec(s, lambda i: (0,) * len(s))
    return pl.pallas_call(
        functools.partial(recurrence_kernel, heads),
        grid=(rows // span,),
        in_specs=[tile(width), tile(width), tile(values.shape[1]), full(1, width), tile(heads),
                  full(*sums.shape)],
        out_specs=[tile(values.shape[1]), tile(width), full(heads, val + TAIL, key)],
        out_shape=[
            jax.ShapeDtypeStruct((rows, values.shape[1]), jnp.float32),
            jax.ShapeDtypeStruct((rows, width), jnp.bfloat16),
            jax.ShapeDtypeStruct((heads, val + TAIL, key), jnp.bfloat16),
        ],
        scratch_shapes=[pltpu.VMEM((heads, val, key), jnp.float32), pltpu.VMEM((1, width), jnp.float32)],
        cost_estimate=pl.CostEstimate(flops=12 * 10**9, bytes_accessed=4 * 10**6, transcendentals=0),
        name="recurrence",
    )(queries, forget, values, floor[None, :], surge, sums)


def mixer_finish(part, decayed, gate, gain, ends):
    rows, width = part.shape
    heads = ends.shape[1]
    val, key = ends.shape[2] - TAIL, ends.shape[3]
    span = SPAN
    tile = lambda w: pl.BlockSpec((span, w), lambda i: (i, 0))
    full = lambda *s: pl.BlockSpec(s, lambda i: (0,) * len(s))
    return pl.pallas_call(
        functools.partial(finish_kernel, heads),
        grid=(rows // span,),
        in_specs=[tile(width), tile(decayed.shape[1]), tile(width), full(1, val), full(*ends.shape)],
        out_specs=tile(width),
        out_shape=jax.ShapeDtypeStruct((rows, width), jnp.bfloat16),
        scratch_shapes=[pltpu.VMEM((heads, val, key), jnp.bfloat16)],
        cost_estimate=pl.CostEstimate(flops=4 * 10**9, bytes_accessed=4 * 10**6, transcendentals=0),
        name="finish",
    )(part, decayed, gate, gain[None, :], ends)


def expert_kernel(x_ref, gate_ref, up_ref, down_ref, out_ref, rows, hidden, gate_buf, up_buf, down_buf,
                  gate_sem, up_sem, down_sem, row_out, row_in, hid_out, hid_in):
    experts, count, _, depth = rows.shape
    part = hidden.shape[3]
    tile, down_tile = gate_buf.shape[2], down_buf.shape[2]
    tiles, down_tiles = gate_buf.shape[0], down_buf.shape[0]
    me = lax.axis_index("tp")

    def hidden_loads(e, j):
        columns = pl.ds(j * tile, tile)
        return (
            pltpu.make_async_copy(gate_ref.at[e, :, columns], gate_buf.at[j], gate_sem.at[j]),
            pltpu.make_async_copy(up_ref.at[e, :, columns], up_buf.at[j], up_sem.at[j]),
        )

    def down_load(e, j):
        columns = pl.ds(j * down_tile, down_tile)
        return pltpu.make_async_copy(down_ref.at[e, :, columns], down_buf.at[j], down_sem.at[j])

    def peer(d):
        return lax.rem(me + d, count)

    def row_copy(e, d):
        return pltpu.make_async_remote_copy(
            src_ref=x_ref.at[e], dst_ref=rows.at[e, me], send_sem=row_out.at[e, d - 1],
            recv_sem=row_in.at[e, d - 1], device_id={"tp": peer(d)}, device_id_type=MESH,
        )

    def hidden_copy(e, d):
        return pltpu.make_async_remote_copy(
            src_ref=hidden.at[e, me], dst_ref=hidden.at[e, me], send_sem=hid_out.at[e, d - 1],
            recv_sem=hid_in.at[e, d - 1], device_id={"tp": peer(d)}, device_id_type=MESH,
        )

    barrier = pltpu.get_barrier_semaphore()
    for d in range(1, count):
        pl.semaphore_signal(barrier, inc=1, device_id={"tp": peer(d)}, device_id_type=MESH)
    for j in range(tiles):
        for load in hidden_loads(0, j):
            load.start()
    for e in range(experts):
        rows[e, me] = x_ref[e]
    pl.semaphore_wait(barrier, count - 1)
    for e in range(experts):
        for d in range(1, count):
            row_copy(e, d).start()
    for j in range(down_tiles):
        down_load(0, j).start()

    @pl.loop(0, experts)
    def _(e):
        for d in range(1, count):
            row_copy(e, d).wait_recv()
        for j in range(tiles):
            for load in hidden_loads(e, j):
                load.wait()
            gate, up = 0.0, 0.0
            for s in range(count):
                piece = rows[e, s]
                gate += dot(piece, gate_buf[j, s * depth:(s + 1) * depth])
                up += dot(piece, up_buf[j, s * depth:(s + 1) * depth])
            hidden[e, me, :, j * tile:(j + 1) * tile] = (jax.nn.silu(gate) * up).astype(jnp.bfloat16)

            @pl.when(e < experts - 1)
            def _():
                for load in hidden_loads(e + 1, j):
                    load.start()

        for d in range(1, count):
            hidden_copy(e, d).start()

    @pl.loop(0, experts)
    def _(e):
        for d in range(1, count):
            hidden_copy(e, d).wait_recv()
        for j in range(down_tiles):
            down_load(e, j).wait()
            total = 0.0
            for s in range(count):
                total += dot(hidden[e, s], down_buf[j, s * part:(s + 1) * part])
            out_ref[e, :, j * down_tile:(j + 1) * down_tile] = total.astype(jnp.bfloat16)

            @pl.when(e < experts - 1)
            def _():
                down_load(e + 1, j).start()

    @pl.loop(0, experts)
    def _(e):
        for d in range(1, count):
            row_copy(e, d).wait_send()
            hidden_copy(e, d).wait_send()


def expert_layer(arrived, gate, up, down):
    experts, slots, depth = arrived.shape
    count = lax.axis_size("tp")
    part, width = gate.shape[2], down.shape[2]
    tile, down_tile = min(256, part), min(256, width)
    vmem = pl.BlockSpec(memory_space=pltpu.VMEM)
    hbm = pl.BlockSpec(memory_space=pl.ANY)
    dma = pltpu.SemaphoreType.DMA
    size = gate.size + up.size + down.size
    return pl.pallas_call(
        expert_kernel,
        in_specs=[vmem, hbm, hbm, hbm],
        out_specs=vmem,
        out_shape=jax.ShapeDtypeStruct((experts, slots, width), jnp.bfloat16),
        scratch_shapes=[
            pltpu.VMEM((experts, count, slots, depth), jnp.bfloat16),
            pltpu.VMEM((experts, count, slots, part), jnp.bfloat16),
            pltpu.VMEM((part // tile, gate.shape[1], tile), jnp.bfloat16),
            pltpu.VMEM((part // tile, up.shape[1], tile), jnp.bfloat16),
            pltpu.VMEM((width // down_tile, down.shape[1], down_tile), jnp.bfloat16),
            dma((part // tile,)), dma((part // tile,)), dma((width // down_tile,)),
        ] + [dma((experts, count - 1))] * 4,
        compiler_params=pltpu.CompilerParams(
            collective_id=1, has_side_effects=True, vmem_limit_bytes=36 * 2**20
        ),
        cost_estimate=pl.CostEstimate(
            flops=4 * slots * size, bytes_accessed=4 * size, transcendentals=0
        ),
        name="experts",
    )(arrived, gate, up, down)


def token_mixing_layer(
    recurrence_queries,
    forget_preact,
    recurrence_values,
    output_gate_preact,
    forget_floor_logits,
    surge_log_decay,
    head_norm_gain,
):
    part, decayed, ending = mixer_part(
        recurrence_queries, forget_preact, recurrence_values, forget_floor_logits, surge_log_decay
    )
    ends = lax.all_gather(ending, "ep")
    gated_heads = mixer_finish(part, decayed, output_gate_preact, head_norm_gain, ends)
    return gated_heads


def mixer_project(gated_heads, recurrence_out_weight):
    return jnp.dot(
        lax.all_gather(gated_heads, "tp", axis=1, tiled=True),
        recurrence_out_weight,
        preferred_element_type=jnp.float32,
    ).astype(jnp.bfloat16)


def routed_experts(
    gated_heads,
    second_micro_rows,
    expert_norm_gain,
    row_group_index,
    group_expert_index,
    chosen_expert_weight,
    expert_gate_weight,
    expert_up_weight,
    expert_down_weight,
):
    row_count = second_micro_rows.shape[0]
    model_width = second_micro_rows.shape[1]
    columns = model_width // lax.axis_size("tp")
    local_count = expert_gate_weight.shape[0]
    expert_count = local_count * lax.axis_size("ep")
    per_group = expert_count // GROUPS
    rows_float = second_micro_rows.astype(jnp.float32)
    normed_rows = (
        rows_float
        * lax.rsqrt(jnp.mean(rows_float * rows_float, axis=-1, keepdims=True) + NORM_EPS)
        * expert_norm_gain
    ).astype(jnp.bfloat16)
    flat_expert = (row_group_index[:, None] * per_group + group_expert_index).reshape(-1)
    onehot = (flat_expert[:, None] == jnp.arange(expert_count, dtype=jnp.int32)[None, :]).astype(
        jnp.int32
    )
    rank_index = jnp.sum((jnp.cumsum(onehot, axis=0) - onehot) * onehot, axis=1)
    slot_index = flat_expert * CAP + rank_index
    owner_row = (
        jnp.full((expert_count * CAP,), row_count, jnp.int32)
        .at[slot_index]
        .set(jnp.arange(2 * row_count) // 2)
    )
    col_part = lax.dynamic_slice_in_dim(normed_rows, lax.axis_index("tp") * columns, columns, 1)
    padded = jnp.concatenate([col_part, jnp.zeros((1, columns), jnp.bfloat16)], axis=0)
    outgoing = padded[owner_row].reshape(expert_count, CAP, columns)
    arrived = lax.all_to_all(outgoing, "ep", split_axis=0, concat_axis=1, tiled=True)
    arrived, _ = lax.optimization_barrier((arrived, gated_heads))
    result = expert_layer(arrived, expert_gate_weight, expert_up_weight, expert_down_weight)
    returned = lax.all_to_all(result, "ep", split_axis=1, concat_axis=0, tiled=True)
    picked = returned.reshape(expert_count * CAP, expert_down_weight.shape[2])[slot_index]
    picked = picked.reshape(row_count, 2, expert_down_weight.shape[2]).astype(jnp.float32)
    return jnp.sum(picked * chosen_expert_weight[:, :, None], axis=1).astype(jnp.bfloat16)


def local(
    recurrence_queries,
    forget_preact,
    recurrence_values,
    output_gate_preact,
    forget_floor_logits,
    surge_log_decay,
    head_norm_gain,
    recurrence_out_weight,
    second_micro_rows,
    expert_norm_gain,
    row_group_index,
    group_expert_index,
    chosen_expert_weight,
    expert_gate_weight,
    expert_up_weight,
    expert_down_weight,
):
    gated_heads = token_mixing_layer(
        recurrence_queries,
        forget_preact,
        recurrence_values,
        output_gate_preact,
        forget_floor_logits,
        surge_log_decay,
        head_norm_gain,
    )
    mixed = mixer_project(gated_heads, recurrence_out_weight)
    expert_out = routed_experts(
        gated_heads,
        second_micro_rows,
        expert_norm_gain,
        row_group_index,
        group_expert_index,
        chosen_expert_weight,
        expert_gate_weight,
        expert_up_weight,
        expert_down_weight,
    )
    return (mixed, expert_out)


def solution(mesh):
    return jax.shard_map(
        local,
        mesh=mesh,
        in_specs=(
            P("ep", "tp"),
            P("ep", "tp"),
            P("ep", "tp"),
            P("ep", "tp"),
            P("tp"),
            P("ep", "tp"),
            P(),
            P(None, "tp"),
            P("ep", None),
            P(),
            P("ep"),
            P("ep", None),
            P("ep", None),
            P("ep", None, "tp"),
            P("ep", None, "tp"),
            P("ep", None, "tp"),
        ),
        out_specs=(P("ep", "tp"), P("ep", "tp")),
        check_vma=False,
    )
```
